32 devices in a mesh: grp: 2 (over y), fs: 4 (over z), tp: 4 (over x, core).
Axes of the slice: x: 2, y: 2, z: 4, core: 2. Of those that a mesh axis runs over, the one named last changes fastest.
Arguments:
- tokens: bfloat16 [2048, 2048], P(('grp', 'fs')), parts along dimension 0, may hold values from -6 to 6
- norm_gain: float32 [2048], P('fs'), may hold values from 0.1 to 1.9
- gate_master: float32 [4, 2048, 1024], P(None, 'fs', 'tp'), may hold values from -0.125 to 0.125
- up_master: float32 [4, 2048, 1024], P(None, 'fs', 'tp'), may hold values from -0.125 to 0.125
- chosen: int32 [2048, 2], P(('grp', 'fs')), parts along dimension 0, may hold values from 0 to 3, all different within a row; in each aligned block of 256 rows (0 to 255, 256 to 511, ...) at most 256 rows name the same one
- affinity: float32 [2048, 2], P(('grp', 'fs')), parts along dimension 0, may hold values from 0.05 to 1
Outputs:
- gate_served: bfloat16 [8, 2048, 1024], P(('grp', 'fs'), None, 'tp'), parts along dimension 0
- up_served: bfloat16 [8, 2048, 1024], P(('grp', 'fs'), None, 'tp'), parts along dimension 0
- hidden: bfloat16 [2048, 2, 1024], P(('grp', 'fs'), None, 'tp'), parts along dimension 0
The draws below stay inside these ranges and needn't reach their ends.
There are 2 independent parts, one for each index of `grp`. The reference program is written for one: setup_inputs(seed, part) draws one part's arguments, and reference() takes and returns one part's arrays. A program takes and returns all parts, laid end to end along the dimension named above; an argument that names none is the same for every part. Nothing has to cross between parts.
Inputs may be any that keep to these rules, and one draw needn't show every extreme that they name: Among the rows of one index of fs (256 tokens, all their choices) no expert is chosen more than 256 times, a bound that some block reaches; the choices of one token differ.
All inputs are finite; a program needn't handle non-finite values.
Results may differ from the reference program's by a relative error of at most 0.023.
Values may be sent and summed in bfloat16 or wider, within the bound.
A program may use at most 64 MiB of HBM per device.

```python
import math
import jax
import jax.numpy as jnp
import numpy as np
from jax import lax

D = 2048
F = 1024
TOP = 2
TOK_DEV = 256
EXPERTS = 4
TOKENS = 1024
CAP = 256
N_FS = 4


def levels(key, dims, shards, least, largest):
    loudness, own = 1.0, jax.random.fold_in(key, 6)
    for axis_at, blocks in shards:
        draws = jnp.exp(jax.random.uniform(jax.random.fold_in(own, axis_at), (blocks,), jnp.float32, least / len(shards), largest / len(shards)))
        loudness = loudness * jnp.repeat(draws, dims[axis_at] // blocks).reshape([-1 if axis == axis_at else 1 for axis in range(len(dims))])
    return loudness


def assign_block(rng, own, number, rows, amount, top, limit, lean):
    ranking = jax.random.permutation(rng, amount)
    crowded, ordinary = shares(amount, rows * top, limit, lean, True), shares(amount, rows * top, limit, lean, False)
    places = jnp.arange(amount)

    def named(tallies, turn):
        used = int((tallies > 0).sum())
        fixed = max(1, used // 4)
        passed = fixed + (places - fixed + turn * (used - fixed)) % max(1, amount - fixed)
        return jnp.zeros((amount,), jnp.int32).at[ranking[jnp.where(places < fixed, places, passed)]].set(jnp.asarray(tallies, jnp.int32))

    tallies = jnp.where(number % 4 == 0, named(crowded, number // 4), named(ordinary, number - number // 4 - 1))
    mixed = jax.random.permutation(jax.random.fold_in(own, 3), amount)
    giver, sink = mixed[0:amount // 2 * 2:2], mixed[1:amount // 2 * 2:2]
    slack = jnp.minimum(tallies[giver] - 1, limit - tallies[sink]) // 2
    slack = jnp.where((giver == ranking[0]) | (sink == ranking[0]) | (tallies[sink] == 0), 0, jnp.maximum(slack, 0))
    passed = jax.random.randint(jax.random.fold_in(own, 4), (amount // 2,), 0, 1 << 20) % (slack + 1)
    tallies = tallies.at[giver].add(-passed).at[sink].add(passed)
    members = jnp.searchsorted(jnp.cumsum(tallies), jnp.arange(rows * top), side="right").astype(jnp.int32)
    table = members.reshape(top, rows).T
    table = table[jax.random.permutation(jax.random.fold_in(own, 1), rows)]
    turn = jax.random.randint(jax.random.fold_in(own, 2), (rows, 1), 0, top)
    return jnp.take_along_axis(table, (jnp.arange(top)[None, :] + turn) % top, axis=1)


def shares(amount, total, most, lean, full):
    weights = [(1 << 20) // math.isqrt(grade ** lean) + 1 for grade in range(1, amount + 1)]
    largest = most if full else min(most, max(-(-total // amount), total * weights[0] // sum(weights)))
    least = 1 if total - largest >= amount - 1 else 0
    counts, rest = [largest] + [least] * (amount - 1), total - largest - least * (amount - 1)
    while rest > 0:
        candidates = [i for i in range(1, amount) if counts[i] < largest] or [i for i in range(1, amount) if counts[i] < most]
        pool, budget = sum([weights[i] for i in candidates]), rest
        for i in candidates:
            extra = min(most - counts[i], max(1, budget * weights[i] // pool), rest)
            counts[i] = counts[i] + extra
            rest = rest - extra
    return np.array(counts)


def bell_draw(own_key, shape, spread, most, split=(), kind=jnp.bfloat16):
    factor_of = levels(own_key, shape, split, -0.22, 0.18) if split else 1.0
    result = jax.random.normal(own_key, shape, jnp.float32) * spread * factor_of
    return jnp.minimum(jnp.maximum(result, -most), most).astype(kind)


def setup_inputs(seed: int = 0, part: int = 0) -> dict:
    key_of = jax.random.split(jax.random.key(seed), 7)
    part_splits = jax.random.split(jax.random.fold_in(key_of[6], part), 7)
    tokens = bell_draw(part_splits[0], (TOKENS, D), 1.0, 6.0, ((0, 4),))
    norm_gain = jnp.clip(1.0 + 0.18 * jax.random.normal(key_of[1], (D,), jnp.float32), 0.1, 1.9)
    gate_master = bell_draw(key_of[2], (EXPERTS, D, F), D ** -0.5, 0.125, ((1, 4), (2, 4)), jnp.float32)
    up_master = bell_draw(key_of[3], (EXPERTS, D, F), D ** -0.5, 0.125, ((1, 4), (2, 4)), jnp.float32)
    chosen_keys = jax.random.split(jax.random.fold_in(part_splits[4], 1), TOKENS // TOK_DEV)
    chosen_turns = jax.random.permutation(jax.random.fold_in(part_splits[4], 3), TOKENS // TOK_DEV)
    chosen = jax.vmap(lambda own, number: assign_block(jax.random.fold_in(part_splits[4], 2), own, number, TOK_DEV, EXPERTS, TOP, CAP, 2))(chosen_keys, chosen_turns).reshape((TOKENS, TOP))
    affinity = jnp.clip(jnp.exp(math.log(1.0) - 2.9957323 * jax.random.uniform(part_splits[5], (TOKENS, TOP), jnp.float32) ** levels(part_splits[5], (TOKENS, TOP), ((0, 4),), -0.2, 0.2)), 0.05, 1.0)
    return {"tokens": tokens, "norm_gain": norm_gain, "gate_master": gate_master, "up_master": up_master, "chosen": chosen, "affinity": affinity}


def reference(tokens, norm_gain, gate_master, up_master, chosen, affinity):
    gate_served = (gate_master * norm_gain[None, :, None]).astype(jnp.bfloat16)
    up_served = (up_master * norm_gain[None, :, None]).astype(jnp.bfloat16)
    xfloat = tokens.astype(jnp.float32)
    scale = lax.rsqrt(lax.optimization_barrier(jnp.mean(xfloat * xfloat, axis=-1)) + 1e-06)
    share = affinity / lax.optimization_barrier(jnp.sum(affinity, axis=-1, keepdims=True))
    blocks = chosen.reshape(N_FS, TOK_DEV * TOP)
    onehot = (blocks[:, :, None] == jnp.arange(EXPERTS, dtype=jnp.int32)[None, None, :]).astype(jnp.int32)
    slot = lax.optimization_barrier(jnp.sum((jnp.cumsum(onehot, axis=1) - onehot) * onehot, axis=2)).astype(jnp.int32)
    source = jnp.arange(N_FS, dtype=jnp.int32)[:, None]
    column = (source * CAP + slot).reshape(-1).astype(jnp.int32)
    owner = (source * TOK_DEV + jnp.repeat(jnp.arange(TOK_DEV, dtype=jnp.int32), TOP)[None, :]).reshape(-1).astype(jnp.int32)
    flat_e = blocks.reshape(-1).astype(jnp.int32)
    index_buf = jnp.zeros((EXPERTS, N_FS * CAP), jnp.int32).at[flat_e, column].set(owner)
    share_buf = jnp.zeros((EXPERTS, N_FS * CAP), jnp.float32).at[flat_e, column].set(share.reshape(-1))

    def one_expert(args):
        index, weight, w_gate, w_up = args
        rows = tokens[index]
        factor = scale[index][:, None]
        gate = jnp.dot(rows, w_gate, preferred_element_type=jnp.float32) * factor
        up = jnp.dot(rows, w_up, preferred_element_type=jnp.float32) * factor
        return (weight[:, None] * jax.nn.silu(gate) * up).astype(jnp.bfloat16)
    hidden_buf = lax.map(one_expert, (index_buf, share_buf, gate_served, up_served))
    hidden = hidden_buf[flat_e, column].reshape(TOKENS, TOP, F)
    return (gate_served, up_served, hidden)
```

```python
import functools

import jax
import jax.numpy as jnp
from jax import lax
from jax.experimental import pallas as pl
from jax.experimental.pallas import tpu as pltpu
from jax.sharding import PartitionSpec as P

MESH = pl.DeviceIdType.MESH
CHUNKS = 2


def routed(tokens, norm_gain, gate_master, up_master, chosen, affinity):
    folded_gate = (gate_master * norm_gain[None, :, None]).astype(jnp.bfloat16)
    folded_up = (up_master * norm_gain[None, :, None]).astype(jnp.bfloat16)
    new_gate, new_up = (
        lax.all_to_all(folded_gate, "fs", split_axis=0, concat_axis=1, tiled=True),
        lax.all_to_all(folded_up, "fs", split_axis=0, concat_axis=1, tiled=True),
    )
    experts_all = gate_master.shape[0]
    tok_rows, width = tokens.shape
    top = chosen.shape[1]
    capacity = tok_rows * top * 2 // experts_all
    local = new_gate.shape[0]
    xfloat = tokens.astype(jnp.float32)
    scale = lax.rsqrt(jnp.mean(xfloat * xfloat, axis=-1) + 1e-06)
    share = affinity / jnp.sum(affinity, axis=-1, keepdims=True)
    flat_e = chosen.reshape(-1)
    onehot = (flat_e[:, None] == jnp.arange(experts_all, dtype=jnp.int32)[None, :]).astype(
        jnp.int32
    )
    slot = jnp.sum((jnp.cumsum(onehot, axis=0) - onehot) * onehot, axis=1)
    target = flat_e * capacity + slot
    owner = jnp.repeat(jnp.arange(tok_rows, dtype=jnp.int32), top)
    total = experts_all * capacity
    scale_buf = (
        jnp.zeros((total,), jnp.float32).at[target].set(scale[owner]).reshape(experts_all, capacity)
    )
    share_buf = (
        jnp.zeros((total,), jnp.float32)
        .at[target]
        .set(share.reshape(-1))
        .reshape(experts_all, capacity)
    )
    narrow = width // lax.axis_size("tp")
    own_cols = lax.dynamic_slice_in_dim(tokens, lax.axis_index("tp") * narrow, narrow, 1)
    row_buf = jnp.zeros((total, narrow), jnp.bfloat16).at[target].set(own_cols[owner])
    row_buf = row_buf.reshape(experts_all, capacity, narrow)
    got_rows, got_scale, got_share = (
        lax.all_to_all(row_buf, "fs", split_axis=0, concat_axis=0, tiled=True),
        lax.all_to_all(
            scale_buf.astype(jnp.bfloat16), "fs", split_axis=0, concat_axis=0, tiled=True
        ).astype(scale_buf.dtype),
        lax.all_to_all(
            share_buf.astype(jnp.bfloat16), "fs", split_axis=0, concat_axis=0, tiled=True
        ).astype(share_buf.dtype),
    )
    sources = got_rows.shape[0] // local
    got_rows = got_rows.reshape(sources, local, capacity, narrow)
    piece = lax.all_gather(got_rows, "tp", axis=3, tiled=True)
    gate = jnp.einsum("secd,edf->secf", piece, new_gate, preferred_element_type=jnp.float32)
    up = jnp.einsum("secd,edf->secf", piece, new_up, preferred_element_type=jnp.float32)
    factor = got_scale.reshape(sources, local, capacity)[..., None]
    weight = got_share.reshape(sources, local, capacity)[..., None]
    gate = gate * factor
    up = up * factor
    hidden_rows = (weight * jax.nn.silu(gate) * up).astype(jnp.bfloat16)
    hidden_rows = hidden_rows.reshape(sources * local, capacity, hidden_rows.shape[3])
    back = lax.all_to_all(hidden_rows, "fs", split_axis=0, concat_axis=0, tiled=True)
    picked = back.reshape(total, back.shape[2])[target].reshape(tok_rows, top, back.shape[2])
    return (new_gate, new_up, picked)


def dense_kernel(
    n, nt, width,
    tok_hbm, gain_ref, gate_hbm, up_hbm, chosen_ref, aff_ref,
    gate_out, up_out, hid_out,
    tok, wf, own, wsend, W, scale, hs, hr,
    ls_tok, ls_w, ls_own, os,
    ss_tz, ss_tx, ss_tm, rs_tok, ss_w, rs_w, ss_y, ss_h, rs_h,
):
    g, z, t = lax.axis_index("grp"), lax.axis_index("fs"), lax.axis_index("tp")
    depth, fcols = wf.shape[1], wf.shape[2]
    fc = fcols // CHUNKS
    mate = t + 1 - 2 * lax.rem(t, 2)
    xq = lax.rem(t + 2, nt)
    xmate = lax.rem(mate + 2, nt)
    rows = tok.shape[2]

    def remote(src, dst, ssem, rsem, **dev):
        return pltpu.make_async_remote_copy(
            src_ref=src, dst_ref=dst, send_sem=ssem, recv_sem=rsem, device_id=dev, device_id_type=MESH
        )

    def tok_load(q):
        return pltpu.make_async_copy(
            tok_hbm.at[:, pl.ds(pl.multiple_of(q * depth, depth), depth)], tok.at[z, q], ls_tok.at[q]
        )

    tok_load(t).start()
    for off in range(1, n):
        e = lax.rem(z + off, n)

        @pl.when(g == 0)
        def _():
            pltpu.make_async_copy(gate_hbm.at[e], wf.at[e], ls_w.at[e]).start()

        @pl.when(g != 0)
        def _():
            pltpu.make_async_copy(up_hbm.at[e], wf.at[e], ls_w.at[e]).start()

    own_loads = [
        pltpu.make_async_copy(gate_hbm.at[z], own.at[0], ls_own.at[0]),
        pltpu.make_async_copy(up_hbm.at[z], own.at[1], ls_own.at[1]),
    ]
    for copy in own_loads:
        copy.start()
    for off in range(1, nt):
        tok_load(lax.rem(t + off, nt)).start()

    barrier = pltpu.get_barrier_semaphore()
    for off in range(1, n):
        pl.semaphore_signal(barrier, 1, device_id={"fs": lax.rem(z + off, n)}, device_id_type=MESH)
    pl.semaphore_signal(barrier, 1, device_id={"grp": 1 - g}, device_id_type=MESH)
    pl.semaphore_signal(barrier, 1, device_id={"tp": mate}, device_id_type=MESH)
    pl.semaphore_signal(barrier, 1, device_id={"tp": xq}, device_id_type=MESH)
    pl.semaphore_wait(barrier, n + 2)

    def tz(s, step):
        return remote(tok.at[s, t], tok.at[s, t], ss_tz.at[s, (step + 1) // 2], rs_tok.at[s, t], fs=z + step)

    def tx(s):
        return remote(tok.at[s, t], tok.at[s, t], ss_tx.at[s], rs_tok.at[s, t], tp=xq)

    def tm(s, q, i):
        return remote(tok.at[s, q], tok.at[s, q], ss_tm.at[s, i], rs_tok.at[s, q], tp=mate)

    def tok_wait(s, q):
        remote(tok.at[s, q], tok.at[s, q], ss_tx.at[s], rs_tok.at[s, q], tp=mate).wait_recv()

    def sides(d, fn):
        for sign in (1, -1):
            s = z + sign * d

            @pl.when((s >= 0) & (s < n))
            def _():
                fn(s, sign)

    tok_load(t).wait()
    sides(1, lambda s, sign: tz(z, sign).start())

    gcol = jnp.transpose(jnp.broadcast_to(gain_ref[...], (128, depth)))
    gcol = jnp.concatenate([gcol] * (fc // 128), axis=1) if fc > 128 else gcol

    def fold(s, sign):
        pltpu.make_async_copy(gate_hbm.at[s], wf.at[s], ls_w.at[s]).wait()
        for c in range(CHUNKS):
            wsend[s, c] = (wf[s, :, c * fc : (c + 1) * fc] * gcol).astype(jnp.bfloat16)

    def lanes(m):
        return pl.ds(pl.multiple_of(m * fc, fc), fc)

    def wcopy(c, to):
        return remote(wsend.at[to, c], W.at[z, c, :, lanes(g)], ss_w.at[c, to], rs_w.at[g, c, z], fs=to)

    def send_weights(c):
        for d in range(n - 1, 0, -1):
            sides(d, lambda s, sign: wcopy(c, s).start())

    for d in range(n - 1, 0, -1):
        sides(d, fold)
    send_weights(0)

    def out_copy(m, c, s):
        ref = (gate_out, up_out)[m]
        return pltpu.make_async_copy(
            W.at[s, c, :, pl.ds(m * fc, fc)],
            ref.at[0, pl.ds(pl.multiple_of(s * depth, depth), depth), pl.ds(c * fc, fc)],
            os.at[m, c, s],
        )

    for m in range(2):
        own_loads[m].wait()
        for c in range(CHUNKS):
            W[z, c, :, m * fc : (m + 1) * fc] = (own[m, :, c * fc : (c + 1) * fc] * gcol).astype(jnp.bfloat16)

    def arrive(s, sign):
        tok_wait(s, t)
        nxt = z - sign

        @pl.when((nxt >= 0) & (nxt < n))
        def _():
            tz(s, -sign).start()

        tx(s).start()
        tm(s, t, 0).start()

    def xrelay(s, sign):
        tok_wait(s, xq)
        tm(s, xq, 1).start()

    def ycopy(c, s):
        return remote(W.at[s, c, :, lanes(g)], W.at[s, c, :, lanes(g)], ss_y.at[c, s], rs_w.at[g, c, s], grp=1 - g)

    def yforward(c):
        def one(s, sign):
            remote(wsend.at[s, c], W.at[s, c, :, lanes(g)], ss_w.at[c, s], rs_w.at[g, c, s], fs=s).wait_recv()
            ycopy(c, s).start()

        for d in range(1, n):
            sides(d, one)

    def ywait(c):
        def one(s, sign):
            o = 1 - g
            remote(W.at[s, c, :, lanes(o)], W.at[s, c, :, lanes(o)], ss_y.at[c, s], rs_w.at[o, c, s], grp=o).wait_recv()

        for d in range(1, n):
            sides(d, one)
        for s in range(n):
            for m in range(2):
                out_copy(m, c, s).start()

    def hcopy(c, to):
        return remote(hs.at[to, c], hr.at[z, c], ss_h.at[c, to], rs_h.at[c, z], fs=to)

    def sumsq(s):
        total = jnp.zeros((rows, 1), jnp.float32)
        for q in range(nt):
            x = tok[s, q].astype(jnp.float32)
            total = total + jnp.sum(x * x, axis=-1, keepdims=True)
        scale[s] = jnp.broadcast_to(lax.rsqrt(total / width + 1e-06), (rows, fc))

    def compute(c):
        def body(i, carry):
            s = lax.rem(z + 1 + i, n)
            acc = jnp.dot(tok[s, 0], W[0, c], preferred_element_type=jnp.float32)
            for q in range(1, nt):
                acc = acc + jnp.dot(tok[s, q], W[q, c], preferred_element_type=jnp.float32)
            gate = acc[:, :fc] * scale[s]
            up = acc[:, fc:] * scale[s]
            h = (gate / (1.0 + jnp.exp(-gate)) * up).astype(jnp.bfloat16)

            @pl.when(s != z)
            def _():
                hs[s, c] = h
                hcopy(c, s).start()

            @pl.when(s == z)
            def _():
                hr[z, c] = h

            return carry

        lax.fori_loop(0, n, body, 0)

    sides(1, arrive)
    sides(2, arrive)
    for c in range(1, CHUNKS):
        send_weights(c)
    sides(1, xrelay)
    yforward(0)
    for d in range(3, n):
        sides(d, arrive)
    for d in range(2, n):
        sides(d, xrelay)
    for off in range(1, nt):
        tok_load(lax.rem(t + off, nt)).wait()
    sumsq(z)

    def rest(s, sign):
        tok_wait(s, mate)
        tok_wait(s, xmate)
        sumsq(s)

    for d in range(1, n):
        sides(d, rest)
    ywait(0)
    compute(0)
    for c in range(1, CHUNKS):
        yforward(c)
        ywait(c)
        compute(c)

    aff = aff_ref[...]
    share = aff / jnp.sum(aff, axis=-1, keepdims=True)
    top = aff.shape[1]
    for c in range(CHUNKS):
        for off in range(1, n):
            s = lax.rem(z + off, n)
            remote(hs.at[s, c], hr.at[s, c], ss_h.at[c, s], rs_h.at[c, s], fs=s).wait_recv()
        for k in range(top):
            ch = jnp.broadcast_to(chosen_ref[:, k : k + 1], (rows, fc))
            picked = jnp.zeros((rows, fc), jnp.float32)
            for e in range(n):
                picked = jnp.where(ch == e, hr[e, c].astype(jnp.float32), picked)
            hid_out[:, k * fcols + c * fc : k * fcols + (c + 1) * fc] = (
                picked * share[:, k : k + 1]
            ).astype(jnp.bfloat16)

    sides(1, lambda s, sign: tz(z, sign).wait_send())

    def drain(s, sign):
        nxt = z - sign

        @pl.when((nxt >= 0) & (nxt < n))
        def _():
            tz(s, -sign).wait_send()

        tx(s).wait_send()
        tm(s, t, 0).wait_send()
        tm(s, xq, 1).wait_send()
        for c in range(CHUNKS):
            wcopy(c, s).wait_send()
            ycopy(c, s).wait_send()
            hcopy(c, s).wait_send()

    for d in range(1, n):
        sides(d, drain)
    for c in range(CHUNKS):
        for s in range(n):
            for m in range(2):
                out_copy(m, c, s).wait()


def dense(tokens, norm_gain, gate_master, up_master, chosen, affinity):
    n, nt = lax.axis_size("fs"), lax.axis_size("tp")
    rows, width = tokens.shape
    experts, depth, fcols = gate_master.shape
    top = chosen.shape[1]
    fc = fcols // CHUNKS
    bf, f32 = jnp.bfloat16, jnp.float32
    dma = pltpu.SemaphoreType.DMA
    any_spec = pl.BlockSpec(memory_space=pl.ANY)
    vmem = pl.BlockSpec(memory_space=pltpu.VMEM)
    gate, up, hid = pl.pallas_call(
        functools.partial(dense_kernel, n, nt, width),
        out_shape=(
            jax.ShapeDtypeStruct((1, width, fcols), bf),
            jax.ShapeDtypeStruct((1, width, fcols), bf),
            jax.ShapeDtypeStruct((rows, top * fcols), bf),
        ),
        in_specs=[any_spec, vmem, any_spec, any_spec, vmem, vmem],
        out_specs=(any_spec, any_spec, vmem),
        scratch_shapes=[
            pltpu.VMEM((n, nt, rows, depth), bf),
            pltpu.VMEM((n, depth, fcols), f32),
            pltpu.VMEM((2, depth, fcols), f32),
            pltpu.VMEM((n, CHUNKS, depth, fc), bf),
            pltpu.VMEM((n, CHUNKS, depth, 2 * fc), bf),
            pltpu.VMEM((n, rows, fc), f32),
            pltpu.VMEM((n, CHUNKS, rows, fc), bf),
            pltpu.VMEM((n, CHUNKS, rows, fc), bf),
            dma((nt,)),
            dma((n,)),
            dma((2,)),
            dma((2, CHUNKS, n)),
            dma((n, 2)),
            dma((n,)),
            dma((n, 2)),
            dma((n, nt)),
            dma((CHUNKS, n)),
            dma((2, CHUNKS, n)),
            dma((CHUNKS, n)),
            dma((CHUNKS, n)),
            dma((CHUNKS, n)),
        ],
        compiler_params=pltpu.CompilerParams(
            collective_id=0, has_side_effects=True, vmem_limit_bytes=48 * 1024 * 1024
        ),
    )(tokens, norm_gain.reshape(1, depth), gate_master, up_master, chosen, affinity)
    return gate, up, hid.reshape(rows, top, fcols)


def on_device(tokens, norm_gain, gate_master, up_master, chosen, affinity):
    n, nt = lax.axis_size("fs"), lax.axis_size("tp")
    experts, depth, fcols = gate_master.shape
    rows, width = tokens.shape
    capacity = rows * chosen.shape[1] * 2 // experts
    fits = (
        experts == n
        and capacity >= rows
        and n >= 3
        and nt == 4
        and lax.axis_size("grp") == 2
        and width == nt * depth
        and fcols % (CHUNKS * 128) == 0
    )
    run = dense if fits else routed
    return run(tokens, norm_gain, gate_master, up_master, chosen, affinity)


def solution(mesh):
    return jax.shard_map(
        on_device,
        mesh=mesh,
        in_specs=(
            P(("grp", "fs"), None),
            P("fs"),
            P(None, "fs", "tp"),
            P(None, "fs", "tp"),
            P(("grp", "fs"), None),
            P(("grp", "fs"), None),
        ),
        out_specs=(
            P(("grp", "fs"), None, "tp"),
            P(("grp", "fs"), None, "tp"),
            P(("grp", "fs"), None, "tp"),
        ),
        check_vma=False,
    )
```

```python
import functools

import jax
import jax.numpy as jnp
from jax import lax
from jax.experimental import pallas as pl
from jax.experimental.pallas import tpu as pltpu
from jax.sharding import PartitionSpec as P

MESH = pl.DeviceIdType.MESH
CHUNKS = 2
PIECES = 4
HALVES = 2


def routed(tokens, norm_gain, gate_master, up_master, chosen, affinity):
    folded_gate = (gate_master * norm_gain[None, :, None]).astype(jnp.bfloat16)
    folded_up = (up_master * norm_gain[None, :, None]).astype(jnp.bfloat16)
    new_gate, new_up = (
        lax.all_to_all(folded_gate, "fs", split_axis=0, concat_axis=1, tiled=True),
        lax.all_to_all(folded_up, "fs", split_axis=0, concat_axis=1, tiled=True),
    )
    experts_all = gate_master.shape[0]
    tok_rows, width = tokens.shape
    top = chosen.shape[1]
    capacity = tok_rows * top * 2 // experts_all
    local = new_gate.shape[0]
    xfloat = tokens.astype(jnp.float32)
    scale = lax.rsqrt(jnp.mean(xfloat * xfloat, axis=-1) + 1e-06)
    share = affinity / jnp.sum(affinity, axis=-1, keepdims=True)
    flat_e = chosen.reshape(-1)
    onehot = (flat_e[:, None] == jnp.arange(experts_all, dtype=jnp.int32)[None, :]).astype(
        jnp.int32
    )
    slot = jnp.sum((jnp.cumsum(onehot, axis=0) - onehot) * onehot, axis=1)
    target = flat_e * capacity + slot
    owner = jnp.repeat(jnp.arange(tok_rows, dtype=jnp.int32), top)
    total = experts_all * capacity
    scale_buf = (
        jnp.zeros((total,), jnp.float32).at[target].set(scale[owner]).reshape(experts_all, capacity)
    )
    share_buf = (
        jnp.zeros((total,), jnp.float32)
        .at[target]
        .set(share.reshape(-1))
        .reshape(experts_all, capacity)
    )
    narrow = width // lax.axis_size("tp")
    own_cols = lax.dynamic_slice_in_dim(tokens, lax.axis_index("tp") * narrow, narrow, 1)
    row_buf = jnp.zeros((total, narrow), jnp.bfloat16).at[target].set(own_cols[owner])
    row_buf = row_buf.reshape(experts_all, capacity, narrow)
    got_rows, got_scale, got_share = (
        lax.all_to_all(row_buf, "fs", split_axis=0, concat_axis=0, tiled=True),
        lax.all_to_all(
            scale_buf.astype(jnp.bfloat16), "fs", split_axis=0, concat_axis=0, tiled=True
        ).astype(scale_buf.dtype),
        lax.all_to_all(
            share_buf.astype(jnp.bfloat16), "fs", split_axis=0, concat_axis=0, tiled=True
        ).astype(share_buf.dtype),
    )
    sources = got_rows.shape[0] // local
    got_rows = got_rows.reshape(sources, local, capacity, narrow)
    piece = lax.all_gather(got_rows, "tp", axis=3, tiled=True)
    gate = jnp.einsum("secd,edf->secf", piece, new_gate, preferred_element_type=jnp.float32)
    up = jnp.einsum("secd,edf->secf", piece, new_up, preferred_element_type=jnp.float32)
    factor = got_scale.reshape(sources, local, capacity)[..., None]
    weight = got_share.reshape(sources, local, capacity)[..., None]
    gate = gate * factor
    up = up * factor
    hidden_rows = (weight * jax.nn.silu(gate) * up).astype(jnp.bfloat16)
    hidden_rows = hidden_rows.reshape(sources * local, capacity, hidden_rows.shape[3])
    back = lax.all_to_all(hidden_rows, "fs", split_axis=0, concat_axis=0, tiled=True)
    picked = back.reshape(total, back.shape[2])[target].reshape(tok_rows, top, back.shape[2])
    return (new_gate, new_up, picked)


def dense_kernel(
    n, nt, width,
    tok_hbm, gain_ref, gate_hbm, up_hbm, chosen_ref, aff_ref,
    gate_out, up_out, hid_out,
    tok, wf, own, wsend, W, scale, hs, hr,
    ls_tok, ls_w, ls_own, os,
    ss_tz, ss_tx, ss_tm, rs_tok, ss_w, rs_w, ss_y, ss_h, rs_h,
):
    g, z, t = lax.axis_index("grp"), lax.axis_index("fs"), lax.axis_index("tp")
    depth, fcols = wf.shape[1], wf.shape[2]
    fc = fcols // CHUNKS
    mate = t + 1 - 2 * lax.rem(t, 2)
    xq = lax.rem(t + 2, nt)
    xmate = lax.rem(mate + 2, nt)
    rows = tok.shape[2]

    def remote(src, dst, ssem, rsem, **dev):
        return pltpu.make_async_remote_copy(
            src_ref=src, dst_ref=dst, send_sem=ssem, recv_sem=rsem, device_id=dev, device_id_type=MESH
        )

    def tok_load(q):
        return pltpu.make_async_copy(
            tok_hbm.at[:, pl.ds(pl.multiple_of(q * depth, depth), depth)], tok.at[z, q], ls_tok.at[q]
        )

    tok_load(t).start()
    for off in range(1, n):
        e = lax.rem(z + off, n)

        @pl.when(g == 0)
        def _():
            pltpu.make_async_copy(gate_hbm.at[e], wf.at[e], ls_w.at[e]).start()

        @pl.when(g != 0)
        def _():
            pltpu.make_async_copy(up_hbm.at[e], wf.at[e], ls_w.at[e]).start()

    own_loads = [
        pltpu.make_async_copy(gate_hbm.at[z], own.at[0], ls_own.at[0]),
        pltpu.make_async_copy(up_hbm.at[z], own.at[1], ls_own.at[1]),
    ]
    for copy in own_loads:
        copy.start()
    for off in range(1, nt):
        tok_load(lax.rem(t + off, nt)).start()

    barrier = pltpu.get_barrier_semaphore()
    for off in range(1, n):
        pl.semaphore_signal(barrier, 1, device_id={"fs": lax.rem(z + off, n)}, device_id_type=MESH)
    pl.semaphore_signal(barrier, 1, device_id={"grp": 1 - g}, device_id_type=MESH)
    pl.semaphore_signal(barrier, 1, device_id={"tp": mate}, device_id_type=MESH)
    pl.semaphore_signal(barrier, 1, device_id={"tp": xq}, device_id_type=MESH)
    pl.semaphore_wait(barrier, n + 2)

    def block(s, q, h):
        return tok.at[s, q, pl.ds(h * (rows // HALVES), rows // HALVES)]

    def tz(s, step, h):
        ref = block(s, t, h)
        return remote(ref, ref, ss_tz.at[s, (step + 1) // 2, h], rs_tok.at[s, t, h], fs=z + step)

    def tx(s, h):
        ref = block(s, t, h)
        return remote(ref, ref, ss_tx.at[s, h], rs_tok.at[s, t, h], tp=xq)

    def tm(s, q, i, h):
        ref = block(s, q, h)
        return remote(ref, ref, ss_tm.at[s, i, h], rs_tok.at[s, q, h], tp=mate)

    def tok_wait(s, q, h):
        ref = block(s, q, h)
        remote(ref, ref, ss_tx.at[s, h], rs_tok.at[s, q, h], tp=mate).wait_recv()

    def sides(d, fn):
        for sign in (1, -1):
            s = z + sign * d

            @pl.when((s >= 0) & (s < n))
            def _():
                fn(s, sign)

    tok_load(t).wait()
    for h in range(HALVES):
        sides(1, lambda s, sign: tz(z, sign, h).start())

    gcol = jnp.transpose(jnp.broadcast_to(gain_ref[...], (128, depth)))
    gcol = jnp.concatenate([gcol] * (fc // 128), axis=1) if fc > 128 else gcol

    def fold(s, sign):
        pltpu.make_async_copy(gate_hbm.at[s], wf.at[s], ls_w.at[s]).wait()
        for c in range(CHUNKS):
            wsend[s, c] = (wf[s, :, c * fc : (c + 1) * fc] * gcol).astype(jnp.bfloat16)

    def lanes(m):
        return pl.ds(pl.multiple_of(m * fc, fc), fc)

    def part(p):
        return pl.ds(p * (depth // PIECES), depth // PIECES)

    def wcopy(c, p, to):
        src, dst = wsend.at[to, c, part(p)], W.at[z, c, part(p), lanes(g)]
        return remote(src, dst, ss_w.at[c, p, to], rs_w.at[g, c, p, z], fs=to)

    def send_weights(c):
        for p in range(PIECES):
            for d in range(n - 1, 0, -1):
                sides(d, lambda s, sign: wcopy(c, p, s).start())

    for d in range(n - 1, 0, -1):
        sides(d, fold)
    at_end = (z == 0) | (z == n - 1)


    def out_copy(m, c, s):
        ref = (gate_out, up_out)[m]
        return pltpu.make_async_copy(
            W.at[s, c, :, pl.ds(m * fc, fc)],
            ref.at[0, pl.ds(pl.multiple_of(s * depth, depth), depth), pl.ds(c * fc, fc)],
            os.at[m, c, s],
        )

    for m in range(2):
        own_loads[m].wait()
        for c in range(CHUNKS):
            W[z, c, :, m * fc : (m + 1) * fc] = (own[m, :, c * fc : (c + 1) * fc] * gcol).astype(jnp.bfloat16)

    def arrive_all(d):
        for h in range(HALVES):

            def arrive(s, sign):
                tok_wait(s, t, h)
                nxt = z - sign

                @pl.when((nxt >= 0) & (nxt < n))
                def _():
                    tz(s, -sign, h).start()

                tx(s, h).start()
                tm(s, t, 0, h).start()

            sides(d, arrive)

    def xrelay(s, sign):
        for h in range(HALVES):
            tok_wait(s, xq, h)
            tm(s, xq, 1, h).start()

    def ycopy(c, p, s):
        ref = W.at[s, c, part(p), lanes(g)]
        return remote(ref, ref, ss_y.at[c, p, s], rs_w.at[g, c, p, s], grp=1 - g)

    def yforward(c):
        for p in range(PIECES):

            def one(s, sign):
                src, dst = wsend.at[s, c, part(p)], W.at[s, c, part(p), lanes(g)]
                remote(src, dst, ss_w.at[c, p, s], rs_w.at[g, c, p, s], fs=s).wait_recv()
                ycopy(c, p, s).start()

            for d in range(n - 1, 0, -1):
                sides(d, one)

    def ywait(c):
        def one(s, sign):
            o = 1 - g
            for p in range(PIECES):
                ref = W.at[s, c, part(p), lanes(o)]
                remote(ref, ref, ss_y.at[c, p, s], rs_w.at[o, c, p, s], grp=o).wait_recv()

        for d in range(1, n):
            sides(d, one)
        for s in range(n):
            for m in range(2):
                out_copy(m, c, s).start()

    def hcopy(c, to):
        return remote(hs.at[to, c], hr.at[z, c], ss_h.at[c, to], rs_h.at[c, z], fs=to)

    def sumsq(s):
        part = jnp.zeros((rows, 128), jnp.float32)
        for q in range(nt):
            for i in range(depth // 128):
                x = tok[s, q, :, i * 128 : (i + 1) * 128].astype(jnp.float32)
                part = part + x * x
        total = jnp.sum(part, axis=-1, keepdims=True)
        scale[s] = jnp.broadcast_to(lax.rsqrt(total / width + 1e-06), (rows, fc))

    def compute(c):
        def body(i, carry):
            s = lax.rem(z + 1 + i, n)
            acc = jnp.dot(tok[s, 0], W[0, c], preferred_element_type=jnp.float32)
            for q in range(1, nt):
                acc = acc + jnp.dot(tok[s, q], W[q, c], preferred_element_type=jnp.float32)
            gate = acc[:, :fc] * scale[s]
            up = acc[:, fc:] * scale[s]
            h = (gate / (1.0 + jnp.exp(-gate)) * up).astype(jnp.bfloat16)

            @pl.when(s != z)
            def _():
                hs[s, c] = h
                hcopy(c, s).start()

            @pl.when(s == z)
            def _():
                hr[z, c] = h

            return carry

        lax.fori_loop(0, n, body, 0)

    arrive_all(1)

    arrive_all(2)
    send_weights(0)
    sides(1, xrelay)
    for d in range(3, n):
        arrive_all(d)
    for c in range(1, CHUNKS):
        send_weights(c)
    yforward(0)
    for d in range(2, n):
        sides(d, xrelay)
    for off in range(1, nt):
        tok_load(lax.rem(t + off, nt)).wait()
    sumsq(z)

    def rest(s, sign):
        for h in range(HALVES):
            tok_wait(s, mate, h)
            tok_wait(s, xmate, h)
        sumsq(s)

    for d in range(1, n):
        sides(d, rest)
    for c in range(1, CHUNKS):
        yforward(c)
    for c in range(CHUNKS):
        ywait(c)
        compute(c)

    aff = aff_ref[...]
    share = aff / jnp.sum(aff, axis=0, keepdims=True)
    top = aff.shape[0]

    def column(row):
        col = jnp.transpose(jnp.broadcast_to(row, (128, rows)))
        return jnp.concatenate([col] * (fc // 128), axis=1) if fc > 128 else col

    shares = [column(share[k : k + 1, :]) for k in range(top)]
    names = [column(chosen_ref[k : k + 1, :].astype(jnp.float32)) for k in range(top)]
    for c in range(CHUNKS):
        for off in range(1, n):
            s = lax.rem(z + off, n)
            remote(hs.at[s, c], hr.at[s, c], ss_h.at[c, s], rs_h.at[c, s], fs=s).wait_recv()
        for k in range(top):
            picked = jnp.zeros((rows, fc), jnp.float32)
            for e in range(n):
                picked = jnp.where(names[k] == e, hr[e, c].astype(jnp.float32), picked)
            hid_out[:, k * fcols + c * fc : k * fcols + (c + 1) * fc] = (
                picked * shares[k]
            ).astype(jnp.bfloat16)

    for h in range(HALVES):
        sides(1, lambda s, sign: tz(z, sign, h).wait_send())

    def drain(s, sign):
        nxt = z - sign

        for h in range(HALVES):

            @pl.when((nxt >= 0) & (nxt < n))
            def _():
                tz(s, -sign, h).wait_send()

            tx(s, h).wait_send()
            tm(s, t, 0, h).wait_send()
            tm(s, xq, 1, h).wait_send()
        for c in range(CHUNKS):
            for p in range(PIECES):
                wcopy(c, p, s).wait_send()
                ycopy(c, p, s).wait_send()
            hcopy(c, s).wait_send()

    for d in range(1, n):
        sides(d, drain)
    for c in range(CHUNKS):
        for s in range(n):
            for m in range(2):
                out_copy(m, c, s).wait()


def dense(tokens, norm_gain, gate_master, up_master, chosen, affinity):
    n, nt = lax.axis_size("fs"), lax.axis_size("tp")
    rows, width = tokens.shape
    experts, depth, fcols = gate_master.shape
    top = chosen.shape[1]
    fc = fcols // CHUNKS
    bf, f32 = jnp.bfloat16, jnp.float32
    dma = pltpu.SemaphoreType.DMA
    any_spec = pl.BlockSpec(memory_space=pl.ANY)
    hbm = pl.BlockSpec(memory_space=pltpu.HBM)
    vmem = pl.BlockSpec(memory_space=pltpu.VMEM)
    gate, up, hid = pl.pallas_call(
        functools.partial(dense_kernel, n, nt, width),
        out_shape=(
            jax.ShapeDtypeStruct((1, width, fcols), bf),
            jax.ShapeDtypeStruct((1, width, fcols), bf),
            jax.ShapeDtypeStruct((rows, top * fcols), bf),
        ),
        in_specs=[hbm, vmem, hbm, hbm, vmem, vmem],
        out_specs=(any_spec, any_spec, vmem),
        scratch_shapes=[
            pltpu.VMEM((n, nt, rows, depth), bf),
            pltpu.VMEM((n, depth, fcols), f32),
            pltpu.VMEM((2, depth, fcols), f32),
            pltpu.VMEM((n, CHUNKS, depth, fc), bf),
            pltpu.VMEM((n, CHUNKS, depth, 2 * fc), bf),
            pltpu.VMEM((n, rows, fc), f32),
            pltpu.VMEM((n, CHUNKS, rows, fc), bf),
            pltpu.VMEM((n, CHUNKS, rows, fc), bf),
            dma((nt,)),
            dma((n,)),
            dma((2,)),
            dma((2, CHUNKS, n)),
            dma((n, 2, HALVES)),
            dma((n, HALVES)),
            dma((n, 2, HALVES)),
            dma((n, nt, HALVES)),
            dma((CHUNKS, PIECES, n)),
            dma((2, CHUNKS, PIECES, n)),
            dma((CHUNKS, PIECES, n)),
            dma((CHUNKS, n)),
            dma((CHUNKS, n)),
        ],
        compiler_params=pltpu.CompilerParams(
            collective_id=0, has_side_effects=True, vmem_limit_bytes=50 * 1024 * 1024
        ),
    )(tokens, norm_gain.reshape(1, depth), gate_master, up_master, chosen.T, affinity.T)
    return gate, up, hid.reshape(rows, top, fcols)


def on_device(tokens, norm_gain, gate_master, up_master, chosen, affinity):
    n, nt = lax.axis_size("fs"), lax.axis_size("tp")
    experts, depth, fcols = gate_master.shape
    rows, width = tokens.shape
    capacity = rows * chosen.shape[1] * 2 // experts
    fits = (
        experts == n
        and capacity >= rows
        and n >= 3
        and nt == 4
        and lax.axis_size("grp") == 2
        and width == nt * depth
        and fcols % (CHUNKS * 128) == 0
    )
    run = dense if fits else routed
    return run(tokens, norm_gain, gate_master, up_master, chosen, affinity)


def solution(mesh):
    return jax.shard_map(
        on_device,
        mesh=mesh,
        in_specs=(
            P(("grp", "fs"), None),
            P("fs"),
            P(None, "fs", "tp"),
            P(None, "fs", "tp"),
            P(("grp", "fs"), None),
            P(("grp", "fs"), None),
        ),
        out_specs=(
            P(("grp", "fs"), None, "tp"),
            P(("grp", "fs"), None, "tp"),
            P(("grp", "fs"), None, "tp"),
        ),
        check_vma=False,
    )
```

```python
import functools

import jax
import jax.numpy as jnp
from jax import lax
from jax.experimental import pallas as pl
from jax.experimental.pallas import tpu as pltpu
from jax.sharding import PartitionSpec as P

MESH = pl.DeviceIdType.MESH
CHUNKS = 2
PIECES = 4
HALVES = 2


def routed(tokens, norm_gain, gate_master, up_master, chosen, affinity):
    folded_gate = (gate_master * norm_gain[None, :, None]).astype(jnp.bfloat16)
    folded_up = (up_master * norm_gain[None, :, None]).astype(jnp.bfloat16)
    new_gate, new_up = (
        lax.all_to_all(folded_gate, "fs", split_axis=0, concat_axis=1, tiled=True),
        lax.all_to_all(folded_up, "fs", split_axis=0, concat_axis=1, tiled=True),
    )
    experts_all = gate_master.shape[0]
    tok_rows, width = tokens.shape
    top = chosen.shape[1]
    capacity = tok_rows * top * 2 // experts_all
    local = new_gate.shape[0]
    xfloat = tokens.astype(jnp.float32)
    scale = lax.rsqrt(jnp.mean(xfloat * xfloat, axis=-1) + 1e-06)
    share = affinity / jnp.sum(affinity, axis=-1, keepdims=True)
    flat_e = chosen.reshape(-1)
    onehot = (flat_e[:, None] == jnp.arange(experts_all, dtype=jnp.int32)[None, :]).astype(
        jnp.int32
    )
    slot = jnp.sum((jnp.cumsum(onehot, axis=0) - onehot) * onehot, axis=1)
    target = flat_e * capacity + slot
    owner = jnp.repeat(jnp.arange(tok_rows, dtype=jnp.int32), top)
    total = experts_all * capacity
    scale_buf = (
        jnp.zeros((total,), jnp.float32).at[target].set(scale[owner]).reshape(experts_all, capacity)
    )
    share_buf = (
        jnp.zeros((total,), jnp.float32)
        .at[target]
        .set(share.reshape(-1))
        .reshape(experts_all, capacity)
    )
    narrow = width // lax.axis_size("tp")
    own_cols = lax.dynamic_slice_in_dim(tokens, lax.axis_index("tp") * narrow, narrow, 1)
    row_buf = jnp.zeros((total, narrow), jnp.bfloat16).at[target].set(own_cols[owner])
    row_buf = row_buf.reshape(experts_all, capacity, narrow)
    got_rows, got_scale, got_share = (
        lax.all_to_all(row_buf, "fs", split_axis=0, concat_axis=0, tiled=True),
        lax.all_to_all(
            scale_buf.astype(jnp.bfloat16), "fs", split_axis=0, concat_axis=0, tiled=True
        ).astype(scale_buf.dtype),
        lax.all_to_all(
            share_buf.astype(jnp.bfloat16), "fs", split_axis=0, concat_axis=0, tiled=True
        ).astype(share_buf.dtype),
    )
    sources = got_rows.shape[0] // local
    got_rows = got_rows.reshape(sources, local, capacity, narrow)
    piece = lax.all_gather(got_rows, "tp", axis=3, tiled=True)
    gate = jnp.einsum("secd,edf->secf", piece, new_gate, preferred_element_type=jnp.float32)
    up = jnp.einsum("secd,edf->secf", piece, new_up, preferred_element_type=jnp.float32)
    factor = got_scale.reshape(sources, local, capacity)[..., None]
    weight = got_share.reshape(sources, local, capacity)[..., None]
    gate = gate * factor
    up = up * factor
    hidden_rows = (weight * jax.nn.silu(gate) * up).astype(jnp.bfloat16)
    hidden_rows = hidden_rows.reshape(sources * local, capacity, hidden_rows.shape[3])
    back = lax.all_to_all(hidden_rows, "fs", split_axis=0, concat_axis=0, tiled=True)
    picked = back.reshape(total, back.shape[2])[target].reshape(tok_rows, top, back.shape[2])
    return (new_gate, new_up, picked)


def dense_kernel(
    n, nt, width,
    tok_hbm, gain_ref, gate_hbm, up_hbm, chosen_ref, aff_ref,
    gate_out, up_out, hid_out,
    tok, wf, own, wsend, W, scale, hs, hr,
    ls_tok, ls_w, ls_own, os,
    ss_tz, ss_tx, ss_tm, rs_tok, ss_w, rs_w, ss_y, ss_h, rs_h,
):
    g, z, t = lax.axis_index("grp"), lax.axis_index("fs"), lax.axis_index("tp")
    depth, fcols = wf.shape[1], wf.shape[2]
    fc = fcols // CHUNKS
    mate = t + 1 - 2 * lax.rem(t, 2)
    xq = lax.rem(t + 2, nt)
    xmate = lax.rem(mate + 2, nt)
    rows = tok.shape[2]

    def remote(src, dst, ssem, rsem, **dev):
        return pltpu.make_async_remote_copy(
            src_ref=src, dst_ref=dst, send_sem=ssem, recv_sem=rsem, device_id=dev, device_id_type=MESH
        )

    def tok_load(q):
        return pltpu.make_async_copy(
            tok_hbm.at[:, pl.ds(pl.multiple_of(q * depth, depth), depth)], tok.at[z, q], ls_tok.at[q]
        )

    tok_load(t).start()
    for off in range(1, n):
        e = lax.rem(z + off, n)

        @pl.when(g == 0)
        def _():
            pltpu.make_async_copy(gate_hbm.at[e], wf.at[e], ls_w.at[e]).start()

        @pl.when(g != 0)
        def _():
            pltpu.make_async_copy(up_hbm.at[e], wf.at[e], ls_w.at[e]).start()

    own_loads = [
        pltpu.make_async_copy(gate_hbm.at[z], own.at[0], ls_own.at[0]),
        pltpu.make_async_copy(up_hbm.at[z], own.at[1], ls_own.at[1]),
    ]
    for copy in own_loads:
        copy.start()
    for off in range(1, nt):
        tok_load(lax.rem(t + off, nt)).start()

    barrier = pltpu.get_barrier_semaphore()
    for off in range(1, n):
        pl.semaphore_signal(barrier, 1, device_id={"fs": lax.rem(z + off, n)}, device_id_type=MESH)
    pl.semaphore_signal(barrier, 1, device_id={"grp": 1 - g}, device_id_type=MESH)
    pl.semaphore_signal(barrier, 1, device_id={"tp": mate}, device_id_type=MESH)
    pl.semaphore_signal(barrier, 1, device_id={"tp": xq}, device_id_type=MESH)
    pl.semaphore_wait(barrier, n + 2)

    def block(s, q, h):
        return tok.at[s, q, pl.ds(h * (rows // HALVES), rows // HALVES)]

    def tz(s, step, h):
        ref = block(s, t, h)
        return remote(ref, ref, ss_tz.at[s, (step + 1) // 2, h], rs_tok.at[s, t, h], fs=z + step)

    def tx(s, h):
        ref = block(s, t, h)
        return remote(ref, ref, ss_tx.at[s, h], rs_tok.at[s, t, h], tp=xq)

    def tm(s, q, i, h):
        ref = block(s, q, h)
        return remote(ref, ref, ss_tm.at[s, i, h], rs_tok.at[s, q, h], tp=mate)

    def tok_wait(s, q, h):
        ref = block(s, q, h)
        remote(ref, ref, ss_tx.at[s, h], rs_tok.at[s, q, h], tp=mate).wait_recv()

    def sides(d, fn):
        for sign in (1, -1):
            s = z + sign * d

            @pl.when((s >= 0) & (s < n))
            def _():
                fn(s, sign)

    tok_load(t).wait()
    for h in range(HALVES):
        sides(1, lambda s, sign: tz(z, sign, h).start())

    gcol = jnp.transpose(jnp.broadcast_to(gain_ref[...], (128, depth)))
    gcol = jnp.concatenate([gcol] * (fc // 128), axis=1) if fc > 128 else gcol

    def fold(s, sign):
        pltpu.make_async_copy(gate_hbm.at[s], wf.at[s], ls_w.at[s]).wait()
        for c in range(CHUNKS):
            wsend[s, c] = (wf[s, :, c * fc : (c + 1) * fc] * gcol).astype(jnp.bfloat16)

    def lanes(m):
        return pl.ds(pl.multiple_of(m * fc, fc), fc)

    def part(p):
        return pl.ds(p * (depth // PIECES), depth // PIECES)

    def wcopy(c, p, to):
        src, dst = wsend.at[to, c, part(p)], W.at[z, c, part(p), lanes(g)]
        return remote(src, dst, ss_w.at[c, p, to], rs_w.at[g, c, p, z], fs=to)

    def send_weights(c):
        for p in range(PIECES):
            for d in range(n - 1, 0, -1):
                sides(d, lambda s, sign: wcopy(c, p, s).start())

    for d in range(n - 1, 0, -1):
        sides(d, fold)
    at_end = (z == 0) | (z == n - 1)


    def out_copy(m, c, s):
        ref = (gate_out, up_out)[m]
        return pltpu.make_async_copy(
            W.at[s, c, :, pl.ds(m * fc, fc)],
            ref.at[0, pl.ds(pl.multiple_of(s * depth, depth), depth), pl.ds(c * fc, fc)],
            os.at[m, c, s],
        )

    for m in range(2):
        own_loads[m].wait()
        for c in range(CHUNKS):
            W[z, c, :, m * fc : (m + 1) * fc] = (own[m, :, c * fc : (c + 1) * fc] * gcol).astype(jnp.bfloat16)

    def arrive_all(d):
        for h in range(HALVES):

            def arrive(s, sign):
                tok_wait(s, t, h)
                nxt = z - sign

                @pl.when((nxt >= 0) & (nxt < n))
                def _():
                    tz(s, -sign, h).start()

                tx(s, h).start()
                tm(s, t, 0, h).start()

            sides(d, arrive)

    def xrelay(s, sign):
        for h in range(HALVES):
            tok_wait(s, xq, h)
            tm(s, xq, 1, h).start()

    def ycopy(c, p, s):
        ref = W.at[s, c, part(p), lanes(g)]
        return remote(ref, ref, ss_y.at[c, p, s], rs_w.at[g, c, p, s], grp=1 - g)

    def yforward(c):
        for p in range(PIECES):

            def one(s, sign):
                src, dst = wsend.at[s, c, part(p)], W.at[s, c, part(p), lanes(g)]
                remote(src, dst, ss_w.at[c, p, s], rs_w.at[g, c, p, s], fs=s).wait_recv()
                ycopy(c, p, s).start()

            for d in range(n - 1, 0, -1):
                sides(d, one)

    def ywait(c):
        def one(s, sign):
            o = 1 - g
            for p in range(PIECES):
                ref = W.at[s, c, part(p), lanes(o)]
                remote(ref, ref, ss_y.at[c, p, s], rs_w.at[o, c, p, s], grp=o).wait_recv()

        for d in range(1, n):
            sides(d, one)
        for s in range(n):
            for m in range(2):
                out_copy(m, c, s).start()

    def hcopy(c, to):
        return remote(hs.at[to, c], hr.at[z, c], ss_h.at[c, to], rs_h.at[c, z], fs=to)

    def sumsq(s):
        part = jnp.zeros((rows, 128), jnp.float32)
        for q in range(nt):
            for i in range(depth // 128):
                x = tok[s, q, :, i * 128 : (i + 1) * 128].astype(jnp.float32)
                part = part + x * x
        total = jnp.sum(part, axis=-1, keepdims=True)
        scale[s] = jnp.broadcast_to(lax.rsqrt(total / width + 1e-06), (rows, fc))

    def compute(c):
        def body(i, carry):
            s = lax.rem(z + 1 + i, n)
            acc = jnp.dot(tok[s, 0], W[0, c], preferred_element_type=jnp.float32)
            for q in range(1, nt):
                acc = acc + jnp.dot(tok[s, q], W[q, c], preferred_element_type=jnp.float32)
            gate = acc[:, :fc] * scale[s]
            up = acc[:, fc:] * scale[s]
            h = (gate / (1.0 + jnp.exp(-gate)) * up).astype(jnp.bfloat16)

            @pl.when(s != z)
            def _():
                hs[s, c] = h
                hcopy(c, s).start()

            @pl.when(s == z)
            def _():
                hr[z, c] = h

            return carry

        lax.fori_loop(0, n, body, 0)

    arrive_all(1)

    arrive_all(2)
    send_weights(0)
    sides(1, xrelay)
    for d in range(3, n):
        arrive_all(d)
    for c in range(1, CHUNKS):
        send_weights(c)
    yforward(0)
    for d in range(2, n):
        sides(d, xrelay)
    for off in range(1, nt):
        tok_load(lax.rem(t + off, nt)).wait()
    sumsq(z)

    def rest(s, sign):
        for h in range(HALVES):
            tok_wait(s, mate, h)
            tok_wait(s, xmate, h)
        sumsq(s)

    for d in range(1, n):
        sides(d, rest)
    for c in range(1, CHUNKS):
        yforward(c)
    for c in range(CHUNKS):
        ywait(c)
        compute(c)

    aff = aff_ref[...]
    share = aff / jnp.sum(aff, axis=0, keepdims=True)
    top = aff.shape[0]

    def column(row):
        col = jnp.transpose(jnp.broadcast_to(row, (128, rows)))
        return jnp.concatenate([col] * (fc // 128), axis=1) if fc > 128 else col

    shares = [column(share[k : k + 1, :]) for k in range(top)]
    names = [column(chosen_ref[k : k + 1, :].astype(jnp.float32)) for k in range(top)]
    for c in range(CHUNKS):
        for off in range(1, n):
            s = lax.rem(z + off, n)
            remote(hs.at[s, c], hr.at[s, c], ss_h.at[c, s], rs_h.at[c, s], fs=s).wait_recv()
        for k in range(top):
            picked = jnp.zeros((rows, fc), jnp.float32)
            for e in range(n):
                picked = jnp.where(names[k] == e, hr[e, c].astype(jnp.float32), picked)
            hid_out[:, k * fcols + c * fc : k * fcols + (c + 1) * fc] = (
                picked * shares[k]
            ).astype(jnp.bfloat16)

    for h in range(HALVES):
        sides(1, lambda s, sign: tz(z, sign, h).wait_send())

    def drain(s, sign):
        nxt = z - sign

        for h in range(HALVES):

            @pl.when((nxt >= 0) & (nxt < n))
            def _():
                tz(s, -sign, h).wait_send()

            tx(s, h).wait_send()
            tm(s, t, 0, h).wait_send()
            tm(s, xq, 1, h).wait_send()
        for c in range(CHUNKS):
            for p in range(PIECES):
                wcopy(c, p, s).wait_send()
                ycopy(c, p, s).wait_send()
            hcopy(c, s).wait_send()

    for d in range(1, n):
        sides(d, drain)
    for c in range(CHUNKS):
        for s in range(n):
            for m in range(2):
                out_copy(m, c, s).wait()


def dense(tokens, norm_gain, gate_master, up_master, chosen, affinity):
    n, nt = lax.axis_size("fs"), lax.axis_size("tp")
    rows, width = tokens.shape
    experts, depth, fcols = gate_master.shape
    top = chosen.shape[1]
    fc = fcols // CHUNKS
    bf, f32 = jnp.bfloat16, jnp.float32
    dma = pltpu.SemaphoreType.DMA
    any_spec = pl.BlockSpec(memory_space=pl.ANY)
    hbm = pl.BlockSpec(memory_space=pltpu.HBM)
    vmem = pl.BlockSpec(memory_space=pltpu.VMEM)
    gate, up, hid = pl.pallas_call(
        functools.partial(dense_kernel, n, nt, width),
        out_shape=(
            jax.ShapeDtypeStruct((1, width, fcols), bf),
            jax.ShapeDtypeStruct((1, width, fcols), bf),
            jax.ShapeDtypeStruct((rows, top * fcols), bf),
        ),
        in_specs=[hbm, vmem, hbm, hbm, vmem, vmem],
        out_specs=(any_spec, any_spec, vmem),
        scratch_shapes=[
            pltpu.VMEM((n, nt, rows, depth), bf),
            pltpu.VMEM((n, depth, fcols), f32),
            pltpu.VMEM((2, depth, fcols), f32),
            pltpu.VMEM((n, CHUNKS, depth, fc), bf),
            pltpu.VMEM((n, CHUNKS, depth, 2 * fc), bf),
            pltpu.VMEM((n, rows, fc), f32),
            pltpu.VMEM((n, CHUNKS, rows, fc), bf),
            pltpu.VMEM((n, CHUNKS, rows, fc), bf),
            dma((nt,)),
            dma((n,)),
            dma((2,)),
            dma((2, CHUNKS, n)),
            dma((n, 2, HALVES)),
            dma((n, HALVES)),
            dma((n, 2, HALVES)),
            dma((n, nt, HALVES)),
            dma((CHUNKS, PIECES, n)),
            dma((2, CHUNKS, PIECES, n)),
            dma((CHUNKS, PIECES, n)),
            dma((CHUNKS, n)),
            dma((CHUNKS, n)),
        ],
        compiler_params=pltpu.CompilerParams(
            collective_id=0, has_side_effects=True, vmem_limit_bytes=51 * 1024 * 1024
        ),
    )(tokens, norm_gain.reshape(1, depth), gate_master, up_master, chosen.T, affinity.T)
    return gate, up, hid.reshape(rows, top, fcols)


def on_device(tokens, norm_gain, gate_master, up_master, chosen, affinity):
    n, nt = lax.axis_size("fs"), lax.axis_size("tp")
    experts, depth, fcols = gate_master.shape
    rows, width = tokens.shape
    capacity = rows * chosen.shape[1] * 2 // experts
    fits = (
        experts == n
        and capacity >= rows
        and n >= 3
        and nt == 4
        and lax.axis_size("grp") == 2
        and width == nt * depth
        and fcols % (CHUNKS * 128) == 0
    )
    run = dense if fits else routed
    return run(tokens, norm_gain, gate_master, up_master, chosen, affinity)


def solution(mesh):
    return jax.shard_map(
        on_device,
        mesh=mesh,
        in_specs=(
            P(("grp", "fs"), None),
            P("fs"),
            P(None, "fs", "tp"),
            P(None, "fs", "tp"),
            P(("grp", "fs"), None),
            P(("grp", "fs"), None),
        ),
        out_specs=(
            P(("grp", "fs"), None, "tp"),
            P(("grp", "fs"), None, "tp"),
            P(("grp", "fs"), None, "tp"),
        ),
        check_vma=False,
    )
```
